32 devices in a mesh: ep: 8 (over z, core), tp: 4 (over y, x).
Axes of the slice: x: 2, y: 2, z: 4, core: 2. Of those that a mesh axis runs over, the one named last changes fastest.
Arguments:
- query_vectors: bfloat16 [4096, 4096], P('ep', 'tp'), may hold values from -6 to 6
- key_vectors: bfloat16 [4096, 2048], P('ep', 'tp'), may hold values from -6 to 6
- value_vectors: bfloat16 [4096, 2048], P('ep', 'tp'), may hold values from -64 to 64
- query_gain: float32 [128], replicated, may hold values from 0.1 to 1.9
- key_gain: float32 [128], replicated, may hold values from 0.1 to 1.9
- sink_logits: float32 [32], P('tp'), may hold values from 3 to 7
- moe_rows: bfloat16 [1280, 4096], P('ep', 'tp'), may hold values from -6 to 6
- norm_gain: float32 [4096], replicated, may hold values from 0.1 to 1.9
- expert_ids: int32 [1280, 4], P('ep'), may hold values from 0 to 7, all different within a row; in each aligned block of 160 rows (0 to 159, 160 to 319, ...) at most 120 rows name the same one
- route_weights: float32 [1280, 4], P('ep'), may hold values from 0.25 to 2.5
- expert_gate: bfloat16 [8, 4096, 2048], P('ep', None, 'tp'), may hold values from -0.09375 to 0.09375
- expert_up: bfloat16 [8, 4096, 2048], P('ep', None, 'tp'), may hold values from -0.09375 to 0.09375
- expert_down: bfloat16 [8, 2048, 4096], P('ep', None, 'tp'), may hold values from -0.125 to 0.125
- shared_gate: bfloat16 [4096, 512], P(None, 'tp'), may hold values from -0.09375 to 0.09375
- shared_up: bfloat16 [4096, 512], P(None, 'tp'), may hold values from -0.09375 to 0.09375
- shared_down: bfloat16 [512, 4096], P(None, 'tp'), may hold values from -0.25 to 0.25
Outputs:
- attended: bfloat16 [4096, 4096], P('ep', 'tp')
- moe_out: bfloat16 [1280, 4096], P('ep', 'tp')
The draws below stay inside these ranges and needn't reach their ends.
Inputs may be any that keep to these rules, and one draw needn't show every extreme that they name: `expert_ids`: each row names 4 different experts. Within the rows of one index of ep (aligned blocks of 160 rows), no expert is named by more than 120 rows, and in some block one expert is named by exactly 120.
All inputs are finite; a program needn't handle non-finite values.
Results may differ from the reference program's by a relative error of at most 0.0071.
Values may be sent and summed in bfloat16 or wider, within the bound.
No kernel may reach another device: no remote copies, remote signals or barrier semaphores. Data moves between devices by JAX's collectives and lax.ppermute only.
A program may use at most 128 MiB of HBM per device.

```python
import math
import jax
import jax.numpy as jnp
import numpy as np
from jax import lax

HEAD_DIM = 128
HEADS = 32
KV_HEADS = 16
GROUP = 2
WINDOW = 128
GRID_W = 64
TOK_A = 512
SEQ_A = 4096
D = 4096
F = 2048
FS = 512
TOP_K = 4
TOK_B = 160
TOKENS_B = 1280
EXPERTS = 8
CAP = 120


def levels(stream_key, shape, shards, least, largest):
    def one(position, parts):
        steps = jax.random.uniform(jax.random.fold_in(jax.random.fold_in(stream_key, 6), position), (parts,), jnp.float32, least / len(shards), largest / len(shards))
        return jnp.repeat(jnp.exp(steps), shape[position] // parts).reshape((-1,) + (1,) * (len(shape) - position - 1))

    loudness = one(*shards[0])
    for cut in shards[1:]:
        loudness = loudness * one(*cut)
    return loudness


def shared_out(key, own, number, rows, number_of, top, bound, lean):
    sequence = jax.random.permutation(key, number_of)
    heavy_load, ordinary = portions_of(number_of, rows * top, bound, lean, True), portions_of(number_of, rows * top, bound, lean, False)
    places = jnp.arange(number_of)

    def named(sizes, offset_by):
        used = int((sizes > 0).sum())
        fixed = max(1, used // 4)
        shifted = fixed + (places - fixed + offset_by * (used - fixed)) % max(1, number_of - fixed)
        return jnp.zeros((number_of,), jnp.int32).at[sequence[jnp.where(places < fixed, places, shifted)]].set(jnp.asarray(sizes, jnp.int32))

    sizes = jnp.where(number % 4 == 0, named(heavy_load, number // 4), named(ordinary, number - number // 4 - 1))
    mixed = jax.random.permutation(jax.random.fold_in(own, 3), number_of)
    giver, receiver = mixed[0:number_of // 2 * 2:2], mixed[1:number_of // 2 * 2:2]
    room = jnp.minimum(sizes[giver] - 1, bound - sizes[receiver]) // 2
    room = jnp.where((giver == sequence[0]) | (receiver == sequence[0]) | (sizes[receiver] == 0), 0, jnp.maximum(room, 0))
    shifted = jax.random.randint(jax.random.fold_in(own, 4), (number_of // 2,), 0, 1 << 20) % (room + 1)
    sizes = sizes.at[giver].add(-shifted).at[receiver].add(shifted)
    items = jnp.searchsorted(jnp.cumsum(sizes), jnp.arange(rows * top), side="right").astype(jnp.int32)
    table = items.reshape(top, rows).T
    table = table[jax.random.permutation(jax.random.fold_in(own, 1), rows)]
    offset_by = jax.random.randint(jax.random.fold_in(own, 2), (rows, 1), 0, top)
    return jnp.take_along_axis(table, (jnp.arange(top)[None, :] + offset_by) % top, axis=1)


def portions_of(amount, total, most, skew, full):
    portions = [(1 << 20) // math.isqrt(standing ** skew) + 1 for standing in range(1, amount + 1)]
    largest = most if full else min(most, max(-(-total // amount), total * portions[0] // sum(portions)))
    least = 1 if total - largest >= amount - 1 else 0
    holding, rest = [largest] + [least] * (amount - 1), total - largest - least * (amount - 1)
    while rest > 0:
        free = [i for i in range(1, amount) if holding[i] < largest] or [i for i in range(1, amount) if holding[i] < most]
        pool, budget = sum([portions[i] for i in free]), rest
        for i in free:
            extra = min(most - holding[i], max(1, budget * portions[i] // pool), rest)
            holding[i] = holding[i] + extra
            rest = rest - extra
    return np.array(holding)


def gaussian(own_key, shape, width, reach, cuts=(), kind=jnp.bfloat16):
    result = width * jax.random.normal(own_key, shape, jnp.float32)
    if cuts:
        result = result * levels(own_key, shape, cuts, -0.22, 0.18)
    return jnp.clip(result, -reach, reach).astype(kind)


def setup_inputs(seed: int = 0) -> dict:
    seeds = jax.random.split(jax.random.key(seed), 17)
    query_vectors = gaussian(seeds[0], (SEQ_A, HEADS * HEAD_DIM), 1.0, 6.0, ((0, 8), (1, 4)))
    key_vectors = gaussian(seeds[1], (SEQ_A, KV_HEADS * HEAD_DIM), 1.0, 6.0, ((0, 8), (1, 4)))
    value_vectors = gaussian(seeds[2], (SEQ_A, KV_HEADS * HEAD_DIM), 12.0, 64.0, ((0, 8), (1, 4)))
    query_gain = jnp.clip(1.0 + 0.18 * jax.random.normal(seeds[3], (HEAD_DIM,), jnp.float32), 0.1, 1.9)
    key_gain = jnp.clip(1.0 + 0.18 * jax.random.normal(seeds[4], (HEAD_DIM,), jnp.float32), 0.1, 1.9)
    sink_logits = jnp.clip(3.0 + 4.0 * jax.random.uniform(seeds[5], (HEADS,), jnp.float32) ** levels(seeds[5], (HEADS,), ((0, 4),), -0.2, 0.2), 3.0, 7.0)
    moe_rows = gaussian(seeds[6], (TOKENS_B, D), 1.0, 6.0, ((0, 8), (1, 4)))
    norm_gain = jnp.clip(1.0 + 0.18 * jax.random.normal(seeds[7], (D,), jnp.float32), 0.1, 1.9)
    expert_ids_keys = jax.random.split(jax.random.fold_in(seeds[8], 1), TOKENS_B // TOK_B)
    expert_ids_turns = jax.random.permutation(jax.random.fold_in(seeds[8], 3), TOKENS_B // TOK_B)
    expert_ids = jax.vmap(lambda own, number: shared_out(jax.random.fold_in(seeds[8], 2), own, number, TOK_B, EXPERTS, TOP_K, CAP, 2))(expert_ids_keys, expert_ids_turns).reshape((TOKENS_B, TOP_K))
    route_weights = jnp.clip(jnp.exp(math.log(2.5) - 2.3025851 * jax.random.uniform(seeds[9], (TOKENS_B, TOP_K), jnp.float32) ** levels(seeds[9], (TOKENS_B, TOP_K), ((0, 8),), -0.2, 0.2)), 0.25, 2.5)
    expert_gate = gaussian(seeds[10], (EXPERTS, D, F), D ** -0.5, 0.09375, ((0, 8), (2, 4)))
    expert_up = gaussian(seeds[11], (EXPERTS, D, F), D ** -0.5, 0.09375, ((0, 8), (2, 4)))
    expert_down = gaussian(seeds[12], (EXPERTS, F, D), F ** -0.5, 0.125, ((0, 8), (2, 4)))
    shared_gate = gaussian(seeds[13], (D, FS), D ** -0.5, 0.09375, ((1, 4),))
    shared_up = gaussian(seeds[14], (D, FS), D ** -0.5, 0.09375, ((1, 4),))
    shared_down = gaussian(seeds[15], (FS, D), FS ** -0.5, 0.25, ((1, 4),))
    return dict(query_vectors=query_vectors, key_vectors=key_vectors, value_vectors=value_vectors, query_gain=query_gain, key_gain=key_gain, sink_logits=sink_logits, moe_rows=moe_rows, norm_gain=norm_gain, expert_ids=expert_ids, route_weights=route_weights, expert_gate=expert_gate, expert_up=expert_up, expert_down=expert_down, shared_gate=shared_gate, shared_up=shared_up, shared_down=shared_down)


epsilon = 1e-06
rotary_base = 10000.0

def half_turn(halves):
    leading, trailing = jnp.split(halves, 2, axis=-1)
    return jnp.concatenate([-trailing, leading], axis=-1)

def rotate_heads(vectors, head_gain, positions):
    floats = vectors.astype(jnp.float32)
    normed = floats * lax.rsqrt(lax.optimization_barrier(jnp.mean(floats * floats, axis=-1, keepdims=True)) + epsilon) * head_gain
    quarter = HEAD_DIM // 4
    freq_index = jnp.arange(quarter, dtype=jnp.int32).astype(jnp.float32)
    inverse = rotary_base ** (-4.0 * freq_index / HEAD_DIM)
    grid_row = (positions // GRID_W).astype(jnp.float32)[:, None] * inverse
    grid_col = (positions % GRID_W).astype(jnp.float32)[:, None] * inverse
    angles = jnp.concatenate([grid_row, grid_row, grid_col, grid_col], axis=-1)[:, None, :]
    row_half, col_half = jnp.split(normed, 2, axis=-1)
    turned = jnp.concatenate([half_turn(row_half), half_turn(col_half)], axis=-1)
    return (normed * jnp.cos(angles) + turned * jnp.sin(angles)).astype(jnp.bfloat16)

def activate(block_rows, gate_weight, up_weight, factor):
    gate_sum = jnp.dot(block_rows, gate_weight, preferred_element_type=jnp.float32) * factor[:, None]
    up_sum = jnp.dot(block_rows, up_weight, preferred_element_type=jnp.float32) * factor[:, None]
    return (jax.nn.silu(gate_sum) * up_sum).astype(jnp.bfloat16)

def windowed(query_vectors, key_vectors, value_vectors, query_gain, key_gain, sink_logits):
    positions = jnp.arange(SEQ_A, dtype=jnp.int32)
    queries = rotate_heads(query_vectors.reshape(SEQ_A, HEADS, HEAD_DIM), query_gain, positions)
    turned_keys = rotate_heads(key_vectors.reshape(SEQ_A, KV_HEADS, HEAD_DIM), key_gain, positions)
    values = value_vectors.reshape(SEQ_A, KV_HEADS, HEAD_DIM)
    padding = ((WINDOW, WINDOW), (0, 0), (0, 0))
    padded_keys = jnp.pad(turned_keys, padding)
    padded_values = jnp.pad(values, padding)
    blocks = SEQ_A // TOK_A
    query_blocks = queries.reshape(blocks, TOK_A, KV_HEADS, GROUP, HEAD_DIM)
    sink_scale = jnp.exp(sink_logits).reshape(KV_HEADS, GROUP)
    extent = TOK_A + 2 * WINDOW
    score_scale = HEAD_DIM ** (-0.5)

    def attend_block(packed):
        query_block, block_index = packed
        first_row = (block_index * TOK_A).astype(jnp.int32)
        near_keys = lax.dynamic_slice_in_dim(padded_keys, first_row, extent, 0)
        near_values = lax.dynamic_slice_in_dim(padded_values, first_row, extent, 0)
        query_pos = first_row + jnp.arange(TOK_A, dtype=jnp.int32)
        key_pos = first_row - WINDOW + jnp.arange(extent, dtype=jnp.int32)
        inside = (jnp.abs(query_pos[:, None] - key_pos[None, :]) <= WINDOW) & (key_pos >= 0)[None, :] & (key_pos < SEQ_A)[None, :]
        scores = jnp.einsum('qhgd,khd->hgqk', query_block.astype(jnp.float32), near_keys.astype(jnp.float32)) * score_scale
        raised = jnp.where(inside, jnp.exp(scores), 0.0)
        denominator = sink_scale[:, :, None] + lax.optimization_barrier(jnp.sum(raised, axis=-1))
        weights = (raised / denominator[..., None]).astype(jnp.bfloat16)
        mixed = jnp.einsum('hgqk,khd->qhgd', weights.astype(jnp.float32), near_values.astype(jnp.float32))
        return mixed.astype(jnp.bfloat16).reshape(TOK_A, HEADS * HEAD_DIM)
    outputs = lax.map(attend_block, (query_blocks, jnp.arange(blocks, dtype=jnp.int32)))
    return outputs.reshape(SEQ_A, HEADS * HEAD_DIM)

def moe_layer(moe_rows, norm_gain, expert_ids, route_weights, expert_gate, expert_up, expert_down, shared_gate, shared_up, shared_down):
    floats = moe_rows.astype(jnp.float32)
    inverse_rms = lax.rsqrt(lax.optimization_barrier(jnp.mean(floats * floats, axis=-1)) + epsilon)
    scaled = (floats * norm_gain).astype(jnp.bfloat16)
    shared_hidden = activate(scaled, shared_gate, shared_up, inverse_rms)
    shared_result = jnp.dot(shared_hidden, shared_down, preferred_element_type=jnp.float32)
    blocks = TOKENS_B // TOK_B
    flat_ids = expert_ids.reshape(blocks, TOK_B * TOP_K).astype(jnp.int32)
    onehot = (flat_ids[:, :, None] == jnp.arange(EXPERTS, dtype=jnp.int32)[None, None, :]).astype(jnp.int32)
    slot_index = lax.optimization_barrier(jnp.sum((jnp.cumsum(onehot, axis=1) - onehot) * onehot, axis=-1)).astype(jnp.int32)
    owner_row = jnp.arange(TOK_B * TOP_K, dtype=jnp.int32) // TOP_K
    scaled_blocks = scaled.reshape(blocks, TOK_B, D)
    rms_blocks = inverse_rms.reshape(blocks, TOK_B)
    capacity_index = jnp.arange(CAP, dtype=jnp.int32)

    def one_expert(packed):
        expert, gate_weight, up_weight, down_weight = packed
        matches = (flat_ids == expert)[:, :, None] & (slot_index[:, :, None] == capacity_index[None, None, :])
        present = jnp.any(matches, axis=1)
        source_row = lax.optimization_barrier(jnp.sum(jnp.where(matches, owner_row[None, :, None], 0), axis=1)).astype(jnp.int32)
        picked = jnp.take_along_axis(scaled_blocks, source_row[:, :, None], axis=1)
        picked = jnp.where(present[:, :, None], picked, jnp.zeros((), jnp.bfloat16))
        factor = jnp.where(present, jnp.take_along_axis(rms_blocks, source_row, axis=1), 0.0)
        hidden = activate(picked.reshape(blocks * CAP, D), gate_weight, up_weight, factor.reshape(blocks * CAP))
        return jnp.dot(hidden, down_weight, preferred_element_type=jnp.float32).astype(jnp.bfloat16).reshape(blocks, CAP, D)
    results = lax.map(one_expert, (jnp.arange(EXPERTS, dtype=jnp.int32), expert_gate, expert_up, expert_down))
    block_ids = expert_ids.reshape(blocks, TOK_B, TOP_K).astype(jnp.int32)
    block_slots = slot_index.reshape(blocks, TOK_B, TOP_K)
    source_block = jnp.arange(blocks, dtype=jnp.int32)[:, None, None]
    gathered = results[block_ids, source_block, block_slots]
    routed = lax.optimization_barrier(jnp.sum(route_weights.reshape(blocks, TOK_B, TOP_K, 1) * gathered.astype(jnp.float32), axis=2))
    return (shared_result + routed.reshape(TOKENS_B, D)).astype(jnp.bfloat16)

def reference(query_vectors, key_vectors, value_vectors, query_gain, key_gain, sink_logits, moe_rows, norm_gain, expert_ids, route_weights, expert_gate, expert_up, expert_down, shared_gate, shared_up, shared_down):
    attended = windowed(query_vectors, key_vectors, value_vectors, query_gain, key_gain, sink_logits)
    moe_out = moe_layer(moe_rows, norm_gain, expert_ids, route_weights, expert_gate, expert_up, expert_down, shared_gate, shared_up, shared_down)
    return (attended, moe_out)
```

```python
import jax
import jax.numpy as jnp
from jax import lax
from jax.sharding import PartitionSpec as P

HEAD_DIM = 128
WINDOW = 128
GRID_W = 64
D = 4096
TOP_K = 4


epsilon = 1e-06
rotary_base = 10000.0


def padded_2(block, sides, width):
    for axis, dim in sides:
        count = lax.axis_size(axis)
        forward = [(i, i + 1) for i in range(count - 1)]
        backward = [(target, source) for source, target in forward]
        low = lax.ppermute(
            lax.slice_in_dim(block, block.shape[dim] - width, None, axis=dim), axis, forward
        )
        high = lax.ppermute(lax.slice_in_dim(block, 0, width, axis=dim), axis, backward)
        block = jnp.concatenate([low, block, high], axis=dim)
    return block


def half_turn(halves):
    leading, trailing = jnp.split(halves, 2, axis=-1)
    return jnp.concatenate([-trailing, leading], axis=-1)


def rotate_heads(vectors, head_gain, positions):
    floats = vectors.astype(jnp.float32)
    normed = (
        floats * lax.rsqrt(jnp.mean(floats * floats, axis=-1, keepdims=True) + epsilon) * head_gain
    )
    quarter = HEAD_DIM // 4
    freq_index = jnp.arange(quarter, dtype=jnp.int32).astype(jnp.float32)
    inverse = rotary_base ** (-4.0 * freq_index / HEAD_DIM)
    grid_row = (positions // GRID_W).astype(jnp.float32)[:, None] * inverse
    grid_col = (positions % GRID_W).astype(jnp.float32)[:, None] * inverse
    angles = jnp.concatenate([grid_row, grid_row, grid_col, grid_col], axis=-1)[:, None, :]
    row_half, col_half = jnp.split(normed, 2, axis=-1)
    turned = jnp.concatenate([half_turn(row_half), half_turn(col_half)], axis=-1)
    return (normed * jnp.cos(angles) + turned * jnp.sin(angles)).astype(jnp.bfloat16)


def attend_window(query_vectors, key_vectors, value_vectors, query_gain, key_gain, sink_logits):
    length = query_vectors.shape[0]
    heads_here = sink_logits.shape[0]
    kv_here = key_vectors.shape[1] // HEAD_DIM
    grouping = heads_here // kv_here
    shard_start = lax.axis_index("ep") * length
    positions = shard_start + jnp.arange(length, dtype=jnp.int32)
    queries = rotate_heads(
        query_vectors.reshape(length, heads_here, HEAD_DIM), query_gain, positions
    )
    turned_keys = rotate_heads(key_vectors.reshape(length, kv_here, HEAD_DIM), key_gain, positions)
    turned_keys = turned_keys.reshape(length, kv_here * HEAD_DIM)
    padded = padded_2(jnp.stack([turned_keys, value_vectors]), (("ep", 1),), WINDOW)
    extent = length + 2 * WINDOW
    near_keys = padded[0].reshape(extent, kv_here, HEAD_DIM)
    near_values = padded[1].reshape(extent, kv_here, HEAD_DIM)
    key_pos = shard_start - WINDOW + jnp.arange(extent, dtype=jnp.int32)
    inside = (
        (jnp.abs(positions[:, None] - key_pos[None, :]) <= WINDOW)
        & (key_pos >= 0)[None, :]
        & (key_pos < lax.axis_size("ep") * length)[None, :]
    )
    scores = jnp.einsum(
        "qhgd,khd->hgqk",
        queries.reshape(length, kv_here, grouping, HEAD_DIM),
        near_keys,
        preferred_element_type=jnp.float32,
    ) * HEAD_DIM ** (-0.5)
    raised = jnp.where(inside, jnp.exp(scores), 0.0)
    denominator = jnp.exp(sink_logits).reshape(kv_here, grouping)[:, :, None] + jnp.sum(
        raised, axis=-1
    )
    weights = (raised / denominator[..., None]).astype(jnp.bfloat16)
    mixed = jnp.einsum("hgqk,khd->qhgd", weights, near_values, preferred_element_type=jnp.float32)
    return mixed.astype(jnp.bfloat16).reshape(length, heads_here * HEAD_DIM)


def project(block_rows, gain_piece, gate_rows, up_rows):
    floats = block_rows.astype(jnp.float32)
    weighted = (floats * gain_piece).astype(jnp.bfloat16)
    gate_sum = jnp.dot(weighted, gate_rows, preferred_element_type=jnp.float32)
    up_sum = jnp.dot(weighted, up_rows, preferred_element_type=jnp.float32)
    return (gate_sum, up_sum, jnp.sum(floats * floats, axis=1))


def activate(gate_sum, up_sum, squares):
    factor = lax.rsqrt(squares / D + epsilon)[:, None]
    return (jax.nn.silu(gate_sum * factor) * (up_sum * factor)).astype(jnp.bfloat16)


def routed_layer(
    moe_rows,
    norm_gain,
    expert_ids,
    route_weights,
    expert_gate,
    expert_up,
    expert_down,
    shared_gate,
    shared_up,
    shared_down,
):
    ep_size = lax.axis_size("ep")
    tokens_here, width_here = moe_rows.shape
    capacity = max(2, 3 * tokens_here * TOP_K // (2 * ep_size))
    slots_all = ep_size * capacity
    flat_ids = expert_ids.reshape(-1)
    onehot = (flat_ids[:, None] == jnp.arange(ep_size, dtype=jnp.int32)[None, :]).astype(jnp.int32)
    slot_index = jnp.sum((jnp.cumsum(onehot, axis=0) - onehot) * onehot, axis=1)
    target = flat_ids * capacity + slot_index
    matches = target[None, :] == jnp.arange(slots_all, dtype=jnp.int32)[:, None]
    present = jnp.any(matches, axis=1)
    owner_row = jnp.arange(tokens_here * TOP_K, dtype=jnp.int32) // TOP_K
    source_row = jnp.sum(jnp.where(matches, owner_row[None, :], 0), axis=1)
    local_gate = expert_gate[0]
    local_up = expert_up[0]
    local_down = expert_down[0]
    units_here = local_gate.shape[1]
    shared_units = shared_gate.shape[1]
    outgoing = jnp.where(
        present[:, None], jnp.take(moe_rows, source_row, axis=0), jnp.zeros((), jnp.bfloat16)
    )
    arrived = lax.all_to_all(
        outgoing.reshape(ep_size, capacity, width_here),
        "ep",
        split_axis=0,
        concat_axis=0,
        tiled=True,
    )
    arrived = arrived.reshape(slots_all, width_here)
    routed = project(
        lax.all_gather(arrived, "tp", axis=1, tiled=True), norm_gain, local_gate, local_up
    )
    shared = project(
        lax.all_gather(moe_rows, "tp", axis=1, tiled=True), norm_gain, shared_gate, shared_up
    )
    gate_sum, up_sum, squares, shared_gsum, shared_usum, own_squares = tuple(
        (new_term for new_term in routed + shared)
    )
    hidden = activate(gate_sum, up_sum, squares)
    shared_hidden = activate(shared_gsum, shared_usum, own_squares)
    packing = units_here // shared_units
    stacked = jnp.concatenate(
        [hidden, shared_hidden.reshape(tokens_here // packing, units_here)], axis=0
    )
    columns = local_down.shape[1]
    portion = lax.all_gather(stacked, "tp", axis=1, tiled=True)
    shards_in = portion.shape[1] // units_here
    routed = jnp.dot(portion[:slots_all], local_down, preferred_element_type=jnp.float32)
    shared_piece = portion[slots_all:].reshape(
        tokens_here // packing, shards_in, packing, shared_units
    )
    shared_piece = shared_piece.transpose(0, 2, 1, 3).reshape(tokens_here, shards_in * shared_units)
    shared = jnp.dot(shared_piece, shared_down, preferred_element_type=jnp.float32)
    returned = lax.all_to_all(
        routed.astype(jnp.bfloat16).reshape(ep_size, capacity, columns),
        "ep",
        split_axis=0,
        concat_axis=0,
        tiled=True,
    )
    returned = returned.reshape(slots_all, columns)
    picked = jnp.take(returned, target, axis=0).reshape(tokens_here, TOP_K, columns)
    combined = shared + jnp.sum(route_weights[:, :, None] * picked.astype(jnp.float32), axis=1)
    return combined.astype(jnp.bfloat16)


def gather_features(piece):
    rows, width = piece.shape
    half = rows // 32 * 16
    place = lax.axis_index("tp")
    side = [(i, i ^ 1) for i in range(4)]
    across = [(i, i ^ 2) for i in range(4)]
    beside = lax.ppermute(piece, "tp", side)
    opposite = lax.ppermute(piece, "tp", across)
    corner_top = lax.ppermute(beside[:half], "tp", across)
    corner_low = lax.ppermute(opposite[half:], "tp", side)
    full = jnp.zeros((rows, 4 * width), piece.dtype)
    full = lax.dynamic_update_slice(full, piece, (0, place * width))
    full = lax.dynamic_update_slice(full, beside, (0, (place ^ 1) * width))
    full = lax.dynamic_update_slice(full, opposite, (0, (place ^ 2) * width))
    full = lax.dynamic_update_slice(full, corner_top, (0, (place ^ 3) * width))
    return lax.dynamic_update_slice(full, corner_low, (half, (place ^ 3) * width))


def dense_layer(
    moe_rows,
    norm_gain,
    expert_ids,
    route_weights,
    expert_gate,
    expert_up,
    expert_down,
    shared_gate,
    shared_up,
    shared_down,
):
    ep_size = lax.axis_size("ep")
    chips = ep_size // 2
    tokens_here = moe_rows.shape[0]
    capacity = max(2, 3 * tokens_here * TOP_K // (2 * ep_size))
    expert = lax.axis_index("ep")
    sibling = [(i, i ^ 1) for i in range(ep_size)]

    def shifted(block, step):
        step = step % chips
        if step == 0:
            return block
        return lax.ppermute(
            block, "ep", [(i, (i + 2 * step) % ep_size) for i in range(ep_size)]
        )

    blocks = [shifted(moe_rows, step) for step in range(chips)]
    routing = jnp.concatenate([expert_ids.astype(jnp.float32).T, route_weights.T], axis=0)
    routing = jnp.stack([shifted(routing, step) for step in range(chips)])
    routing = jnp.stack([routing, lax.ppermute(routing, "ep", sibling)])
    ids = routing[:, :, :TOP_K].astype(jnp.int32)
    factors = routing[:, :, TOP_K:]
    token = jnp.arange(tokens_here, dtype=jnp.int32)
    earlier = (token[:, None] < token[None, :]).astype(jnp.bfloat16)
    slot = jnp.arange(capacity, dtype=jnp.int32)

    def places(wanted, ids):
        named = jnp.any(ids == wanted, axis=2)
        rank = jnp.einsum(
            "jsr,rt->jst", named.astype(jnp.bfloat16), earlier, preferred_element_type=jnp.float32
        ).astype(jnp.int32)
        rank = jnp.where(named, rank, -1)
        return rank[:, :, None, :] == slot[:, None]

    chosen = places(expert, ids)
    chosen_beside = places(expert ^ 1, ids[:1])[0]
    token_factor = jnp.sum(jnp.where(ids == expert, factors, 0.0), axis=2)
    slot_factor = jnp.sum(jnp.where(chosen, token_factor[:, :, None, :], 0.0), axis=3)
    picks = chosen.astype(jnp.bfloat16)
    spread = jnp.concatenate([picks[0], chosen_beside.astype(jnp.bfloat16)], axis=1)
    local_gate = expert_gate[0]
    local_up = expert_up[0]
    local_down = expert_down[0]
    units_here = local_gate.shape[1]
    shared_units = shared_gate.shape[1]
    columns = local_down.shape[1]
    packing = units_here // shared_units
    quarter = tokens_here // packing
    cut = (chips + 1) // 2
    total = None
    for first, last in ((0, cut), (cut, chips)):
        count = last - first
        full = gather_features(jnp.concatenate(blocks[first:last], axis=0))
        both = [full, lax.ppermute(full, "ep", sibling)]
        payload = []
        for side in range(2):
            hidden = activate(*project(both[side], norm_gain, local_gate, local_up))
            payload.append(
                jnp.einsum(
                    "scr,sru->scu",
                    picks[side, first:last],
                    hidden.reshape(count, tokens_here, units_here),
                    preferred_element_type=jnp.float32,
                )
                .astype(jnp.bfloat16)
                .reshape(count * capacity, units_here)
            )
        slots_here = 2 * count * capacity
        if first == 0:
            shared_hidden = activate(
                *project(full[:tokens_here], norm_gain, shared_gate, shared_up)
            )
            payload.append(
                jnp.concatenate(
                    [shared_hidden[i * quarter : (i + 1) * quarter] for i in range(packing)], axis=1
                )
            )
        portion = gather_features(jnp.concatenate(payload, axis=0))
        if first == 0:
            packed = portion[slots_here:]
            pieces = packed.shape[1] // units_here
            shared_piece = jnp.concatenate(
                [
                    jnp.concatenate(
                        [
                            packed[:, (p * packing + i) * shared_units : (p * packing + i + 1) * shared_units]
                            for p in range(pieces)
                        ],
                        axis=1,
                    )
                    for i in range(packing)
                ],
                axis=0,
            )
            shared = jnp.dot(shared_piece, shared_down, preferred_element_type=jnp.float32)
        result = jnp.dot(portion[:slots_here], local_down, preferred_element_type=jnp.float32)
        result = result * slot_factor[:, first:last].reshape(slots_here, 1)
        result = result.astype(jnp.bfloat16).reshape(2, count, capacity, columns)
        crossed = lax.ppermute(result[1], "ep", sibling)
        summed = jnp.einsum(
            "scr,scd->srd",
            spread[first:last],
            jnp.concatenate([result[0], crossed], axis=1),
            preferred_element_type=jnp.float32,
        )
        for step in range(first, last):
            term = summed[step - first]
            if step > 0:
                term = shifted(term.astype(jnp.bfloat16), -step).astype(jnp.float32)
            total = term if total is None else total + term
    return (total + shared).astype(jnp.bfloat16)


def shards(
    query_vectors,
    key_vectors,
    value_vectors,
    query_gain,
    key_gain,
    sink_logits,
    moe_rows,
    norm_gain,
    expert_ids,
    route_weights,
    expert_gate,
    expert_up,
    expert_down,
    shared_gate,
    shared_up,
    shared_down,
):
    attended = attend_window(
        query_vectors, key_vectors, value_vectors, query_gain, key_gain, sink_logits
    )
    moe_args = (
        moe_rows,
        norm_gain,
        expert_ids,
        route_weights,
        expert_gate,
        expert_up,
        expert_down,
        shared_gate,
        shared_up,
        shared_down,
    )
    ep_size = lax.axis_size("ep")
    tokens_here = moe_rows.shape[0]
    few = ep_size * tokens_here <= 3 * tokens_here * TOP_K
    if few and ep_size % 2 == 0 and lax.axis_size("tp") == 4:
        return (attended, dense_layer(*moe_args))
    return (attended, routed_layer(*moe_args))


def solution(mesh):
    placed = (
        P("ep", "tp"),
        P("ep", "tp"),
        P("ep", "tp"),
        P(),
        P(),
        P("tp"),
        P("ep", "tp"),
        P(),
        P("ep", None),
        P("ep", None),
        P("ep", None, "tp"),
        P("ep", None, "tp"),
        P("ep", None, "tp"),
        P(None, "tp"),
        P(None, "tp"),
        P(None, "tp"),
    )
    return jax.shard_map(
        shards,
        mesh=mesh,
        in_specs=placed,
        out_specs=(P("ep", "tp"), P("ep", "tp")),
        check_vma=False,
    )
```

```python
import jax
import jax.numpy as jnp
from jax import lax
from jax.experimental import pallas as pl
from jax.experimental.pallas import tpu as pltpu
from jax.sharding import PartitionSpec as P

HEAD_DIM = 128
WINDOW = 128
GRID_W = 64
D = 4096
TOP_K = 4


epsilon = 1e-06
rotary_base = 10000.0


def attend_kernel(
    start_ref,
    sink_ref,
    q_ref,
    k_ref,
    v_ref,
    low_ref,
    high_ref,
    q_gain_ref,
    k_gain_ref,
    cos_ref,
    sin_ref,
    out_ref,
    keys_ref,
    values_ref,
):
    length = q_ref.shape[0]
    grouping = q_ref.shape[1] // HEAD_DIM
    head = pl.program_id(0)
    lane = lax.broadcasted_iota(jnp.int32, (WINDOW, HEAD_DIM), 1)
    leading = lane % (HEAD_DIM // 2) < HEAD_DIM // 4

    def turn(vectors, gain, row):
        floats = vectors.astype(jnp.float32)
        square = jnp.mean(floats * floats, axis=-1, keepdims=True)
        normed = floats * lax.rsqrt(square + epsilon) * gain
        ahead = pltpu.roll(normed, HEAD_DIM - HEAD_DIM // 4, 1)
        behind = pltpu.roll(normed, HEAD_DIM // 4, 1)
        turned = jnp.where(leading, -ahead, behind)
        cos = cos_ref[row : row + WINDOW, :]
        sin = sin_ref[row : row + WINDOW, :]
        return (normed * cos + turned * sin).astype(jnp.bfloat16)

    k_gain = k_gain_ref[...]
    q_gain = q_gain_ref[...]
    tiles = length // WINDOW
    for i in range(tiles + 2):
        row = i * WINDOW
        if i == 0:
            key, value = low_ref[:WINDOW, :], low_ref[WINDOW:, :]
        elif i == tiles + 1:
            key, value = high_ref[:WINDOW, :], high_ref[WINDOW:, :]
        else:
            key, value = k_ref[row - WINDOW : row, :], v_ref[row - WINDOW : row, :]
        keys_ref[row : row + WINDOW, :] = turn(key, k_gain, row)
        values_ref[row : row + WINDOW, :] = value
    start = start_ref[0]
    total = start_ref[1]
    shape = (grouping * WINDOW, 3 * WINDOW)
    column = lax.broadcasted_iota(jnp.int32, shape, 1)
    offset = column - lax.broadcasted_iota(jnp.int32, shape, 0) % WINDOW
    near = (offset >= 0) & (offset <= 2 * WINDOW)
    sinks = jnp.concatenate(
        [
            jnp.full((WINDOW, 1), sink_ref[head * grouping + g], jnp.float32)
            for g in range(grouping)
        ],
        axis=0,
    )
    for i in range(tiles):
        row = i * WINDOW
        queries = jnp.concatenate(
            [
                turn(
                    q_ref[row : row + WINDOW, g * HEAD_DIM : (g + 1) * HEAD_DIM],
                    q_gain,
                    row + WINDOW,
                )
                for g in range(grouping)
            ],
            axis=0,
        )
        keys = keys_ref[row : row + 3 * WINDOW, :]
        values = values_ref[row : row + 3 * WINDOW, :]
        scores = lax.dot_general(
            queries, keys, (((1,), (1,)), ((), ())), preferred_element_type=jnp.float32
        ) * HEAD_DIM ** (-0.5)
        inside = near
        if i == 0:
            inside = inside & (column + (start - WINDOW) >= 0)
        if i == tiles - 1:
            inside = inside & (column + (start + row - WINDOW) < total)
        raised = jnp.where(inside, jnp.exp(scores), 0.0)
        denominator = sinks + jnp.sum(raised, axis=-1, keepdims=True)
        weights = (raised / denominator).astype(jnp.bfloat16)
        mixed = jnp.dot(weights, values, preferred_element_type=jnp.float32).astype(jnp.bfloat16)
        for g in range(grouping):
            out_ref[row : row + WINDOW, g * HEAD_DIM : (g + 1) * HEAD_DIM] = mixed[
                g * WINDOW : (g + 1) * WINDOW
            ]


def borders(key_vectors, value_vectors):
    length = key_vectors.shape[0]
    count = lax.axis_size("ep")
    forward = [(i, i + 1) for i in range(count - 1)]
    backward = [(target, source) for source, target in forward]
    last = jnp.concatenate([key_vectors[length - WINDOW :], value_vectors[length - WINDOW :]])
    first = jnp.concatenate([key_vectors[:WINDOW], value_vectors[:WINDOW]])
    return lax.ppermute(last, "ep", forward), lax.ppermute(first, "ep", backward)


def attend_window(
    query_vectors, key_vectors, value_vectors, low, high, query_gain, key_gain, sink_logits
):
    length = query_vectors.shape[0]
    heads_here = sink_logits.shape[0]
    kv_here = key_vectors.shape[1] // HEAD_DIM
    grouping = heads_here // kv_here
    extent = length + 2 * WINDOW
    shard_start = lax.axis_index("ep") * length
    positions = shard_start - WINDOW + jnp.arange(extent, dtype=jnp.int32)
    quarter = HEAD_DIM // 4
    freq_index = jnp.arange(quarter, dtype=jnp.int32).astype(jnp.float32)
    inverse = rotary_base ** (-4.0 * freq_index / HEAD_DIM)
    grid_row = (positions // GRID_W).astype(jnp.float32)[:, None] * inverse
    grid_col = (positions % GRID_W).astype(jnp.float32)[:, None] * inverse
    angles = jnp.concatenate([grid_row, grid_col], axis=-1)
    cos_row, cos_col = jnp.split(jnp.cos(angles), 2, axis=-1)
    sin_row, sin_col = jnp.split(jnp.sin(angles), 2, axis=-1)
    cos = jnp.concatenate([cos_row, cos_row, cos_col, cos_col], axis=-1)
    sin = jnp.concatenate([sin_row, sin_row, sin_col, sin_col], axis=-1)
    bounds = jnp.stack([shard_start, lax.axis_size("ep") * length]).astype(jnp.int32)
    whole = lambda h: (0, 0)
    mine = lambda h: (0, h)
    return pl.pallas_call(
        attend_kernel,
        grid=(kv_here,),
        in_specs=[
            pl.BlockSpec(memory_space=pltpu.SMEM),
            pl.BlockSpec(memory_space=pltpu.SMEM),
            pl.BlockSpec((length, grouping * HEAD_DIM), mine),
            pl.BlockSpec((length, HEAD_DIM), mine),
            pl.BlockSpec((length, HEAD_DIM), mine),
            pl.BlockSpec((2 * WINDOW, HEAD_DIM), mine),
            pl.BlockSpec((2 * WINDOW, HEAD_DIM), mine),
            pl.BlockSpec((1, HEAD_DIM), whole),
            pl.BlockSpec((1, HEAD_DIM), whole),
            pl.BlockSpec((extent, HEAD_DIM), whole),
            pl.BlockSpec((extent, HEAD_DIM), whole),
        ],
        out_specs=pl.BlockSpec((length, grouping * HEAD_DIM), mine),
        out_shape=jax.ShapeDtypeStruct(query_vectors.shape, jnp.bfloat16),
        scratch_shapes=[
            pltpu.VMEM((extent, HEAD_DIM), jnp.bfloat16),
            pltpu.VMEM((extent, HEAD_DIM), jnp.bfloat16),
        ],
        cost_estimate=pl.CostEstimate(
            flops=12 * heads_here * length * WINDOW * HEAD_DIM,
            bytes_accessed=6 * length * heads_here * HEAD_DIM,
            transcendentals=3 * heads_here * length * WINDOW,
        ),
        name="attend",
    )(
        bounds,
        jnp.exp(sink_logits),
        query_vectors,
        key_vectors,
        value_vectors,
        low,
        high,
        query_gain[None, :],
        key_gain[None, :],
        cos,
        sin,
    )


def project(block_rows, gain_piece, gate_rows, up_rows):
    floats = block_rows.astype(jnp.float32)
    weighted = (floats * gain_piece).astype(jnp.bfloat16)
    gate_sum = jnp.dot(weighted, gate_rows, preferred_element_type=jnp.float32)
    up_sum = jnp.dot(weighted, up_rows, preferred_element_type=jnp.float32)
    return (gate_sum, up_sum, jnp.sum(floats * floats, axis=1))


def activate(gate_sum, up_sum, squares):
    factor = lax.rsqrt(squares / D + epsilon)[:, None]
    return (jax.nn.silu(gate_sum * factor) * (up_sum * factor)).astype(jnp.bfloat16)


def routed_layer(
    moe_rows,
    norm_gain,
    expert_ids,
    route_weights,
    expert_gate,
    expert_up,
    expert_down,
    shared_gate,
    shared_up,
    shared_down,
):
    ep_size = lax.axis_size("ep")
    tokens_here, width_here = moe_rows.shape
    capacity = max(2, 3 * tokens_here * TOP_K // (2 * ep_size))
    slots_all = ep_size * capacity
    flat_ids = expert_ids.reshape(-1)
    onehot = (flat_ids[:, None] == jnp.arange(ep_size, dtype=jnp.int32)[None, :]).astype(jnp.int32)
    slot_index = jnp.sum((jnp.cumsum(onehot, axis=0) - onehot) * onehot, axis=1)
    target = flat_ids * capacity + slot_index
    matches = target[None, :] == jnp.arange(slots_all, dtype=jnp.int32)[:, None]
    present = jnp.any(matches, axis=1)
    owner_row = jnp.arange(tokens_here * TOP_K, dtype=jnp.int32) // TOP_K
    source_row = jnp.sum(jnp.where(matches, owner_row[None, :], 0), axis=1)
    local_gate = expert_gate[0]
    local_up = expert_up[0]
    local_down = expert_down[0]
    units_here = local_gate.shape[1]
    shared_units = shared_gate.shape[1]
    outgoing = jnp.where(
        present[:, None], jnp.take(moe_rows, source_row, axis=0), jnp.zeros((), jnp.bfloat16)
    )
    arrived = lax.all_to_all(
        outgoing.reshape(ep_size, capacity, width_here),
        "ep",
        split_axis=0,
        concat_axis=0,
        tiled=True,
    )
    arrived = arrived.reshape(slots_all, width_here)
    routed = project(
        lax.all_gather(arrived, "tp", axis=1, tiled=True), norm_gain, local_gate, local_up
    )
    shared = project(
        lax.all_gather(moe_rows, "tp", axis=1, tiled=True), norm_gain, shared_gate, shared_up
    )
    gate_sum, up_sum, squares, shared_gsum, shared_usum, own_squares = tuple(
        (new_term for new_term in routed + shared)
    )
    hidden = activate(gate_sum, up_sum, squares)
    shared_hidden = activate(shared_gsum, shared_usum, own_squares)
    packing = units_here // shared_units
    stacked = jnp.concatenate(
        [hidden, shared_hidden.reshape(tokens_here // packing, units_here)], axis=0
    )
    columns = local_down.shape[1]
    portion = lax.all_gather(stacked, "tp", axis=1, tiled=True)
    shards_in = portion.shape[1] // units_here
    routed = jnp.dot(portion[:slots_all], local_down, preferred_element_type=jnp.float32)
    shared_piece = portion[slots_all:].reshape(
        tokens_here // packing, shards_in, packing, shared_units
    )
    shared_piece = shared_piece.transpose(0, 2, 1, 3).reshape(tokens_here, shards_in * shared_units)
    shared = jnp.dot(shared_piece, shared_down, preferred_element_type=jnp.float32)
    returned = lax.all_to_all(
        routed.astype(jnp.bfloat16).reshape(ep_size, capacity, columns),
        "ep",
        split_axis=0,
        concat_axis=0,
        tiled=True,
    )
    returned = returned.reshape(slots_all, columns)
    picked = jnp.take(returned, target, axis=0).reshape(tokens_here, TOP_K, columns)
    combined = shared + jnp.sum(route_weights[:, :, None] * picked.astype(jnp.float32), axis=1)
    return combined.astype(jnp.bfloat16)


SIDE = [(i, i ^ 1) for i in range(4)]
ACROSS = [(i, i ^ 2) for i in range(4)]


def send_features(piece):
    return piece, lax.ppermute(piece, "tp", SIDE), lax.ppermute(piece, "tp", ACROSS)


def gather_features(sent):
    rows, width = sent[0][0].shape
    half = rows // 32 * 16
    place = lax.axis_index("tp")
    full = jnp.zeros((len(sent) * rows, 4 * width), sent[0][0].dtype)
    for number, (piece, beside, opposite) in enumerate(sent):
        top = number * rows
        corner_top = lax.ppermute(beside[:half], "tp", ACROSS)
        corner_low = lax.ppermute(opposite[half:], "tp", SIDE)
        full = lax.dynamic_update_slice(full, piece, (top, place * width))
        full = lax.dynamic_update_slice(full, beside, (top, (place ^ 1) * width))
        full = lax.dynamic_update_slice(full, opposite, (top, (place ^ 2) * width))
        full = lax.dynamic_update_slice(full, corner_top, (top, (place ^ 3) * width))
        full = lax.dynamic_update_slice(full, corner_low, (top + half, (place ^ 3) * width))
    return full


def dense_layer(
    moe_rows,
    norm_gain,
    expert_ids,
    route_weights,
    expert_gate,
    expert_up,
    expert_down,
    shared_gate,
    shared_up,
    shared_down,
    attend,
):
    ep_size = lax.axis_size("ep")
    chips = ep_size // 2
    tokens_here = moe_rows.shape[0]
    capacity = max(2, 3 * tokens_here * TOP_K // (2 * ep_size))
    expert = lax.axis_index("ep")
    sibling = [(i, i ^ 1) for i in range(ep_size)]

    def shifted(block, step):
        step = step % chips
        if step == 0:
            return block
        return lax.ppermute(
            block, "ep", [(i, (i + 2 * step) % ep_size) for i in range(ep_size)]
        )

    order = sorted(range(chips), key=lambda step: min(step, chips - step))
    sent = [send_features(moe_rows)]
    blocks = [shifted(moe_rows, step) for step in order[1:]]
    sent = sent + [send_features(block) for block in blocks]
    attended = attend(blocks[0])
    routing = jnp.concatenate([expert_ids.astype(jnp.float32).T, route_weights.T], axis=0)
    routing = jnp.stack([shifted(routing, step) for step in order])
    routing = jnp.stack([routing, lax.ppermute(routing, "ep", sibling)])
    ids = routing[:, :, :TOP_K].astype(jnp.int32)
    factors = routing[:, :, TOP_K:]
    token = jnp.arange(tokens_here, dtype=jnp.int32)
    earlier = (token[:, None] < token[None, :]).astype(jnp.bfloat16)
    slot = jnp.arange(capacity, dtype=jnp.int32)

    def places(wanted, ids):
        named = jnp.any(ids == wanted, axis=2)
        rank = jnp.einsum(
            "jsr,rt->jst", named.astype(jnp.bfloat16), earlier, preferred_element_type=jnp.float32
        ).astype(jnp.int32)
        rank = jnp.where(named, rank, -1)
        return rank[:, :, None, :] == slot[:, None]

    chosen = places(expert, ids)
    chosen_beside = places(expert ^ 1, ids[:1])[0]
    token_factor = jnp.sum(jnp.where(ids == expert, factors, 0.0), axis=2)
    slot_factor = jnp.sum(jnp.where(chosen, token_factor[:, :, None, :], 0.0), axis=3)
    picks = chosen.astype(jnp.bfloat16)
    spread = jnp.concatenate([picks[0], chosen_beside.astype(jnp.bfloat16)], axis=1)
    local_gate = expert_gate[0]
    local_up = expert_up[0]
    local_down = expert_down[0]
    units_here = local_gate.shape[1]
    shared_units = shared_gate.shape[1]
    columns = local_down.shape[1]
    packing = units_here // shared_units
    quarter = tokens_here // packing
    cut = (chips + 1) // 2
    groups = ((0, cut), (cut, chips))
    moved = []
    for first, last in groups:
        count = last - first
        full = gather_features(sent[first:last])
        both = [full, lax.ppermute(full, "ep", sibling)]
        payload = []
        for side in range(2):
            hidden = activate(*project(both[side], norm_gain, local_gate, local_up))
            payload.append(
                jnp.einsum(
                    "scr,sru->scu",
                    picks[side, first:last],
                    hidden.reshape(count, tokens_here, units_here),
                    preferred_element_type=jnp.float32,
                )
                .astype(jnp.bfloat16)
                .reshape(count * capacity, units_here)
            )
        if first == 0:
            shared_hidden = activate(
                *project(full[:tokens_here], norm_gain, shared_gate, shared_up)
            )
            payload.append(
                jnp.concatenate(
                    [shared_hidden[i * quarter : (i + 1) * quarter] for i in range(packing)], axis=1
                )
            )
        payload = jnp.concatenate(payload, axis=0)
        if moved:
            piece, beside, opposite = moved[0]
            payload, beside, opposite = lax.optimization_barrier((payload, beside, opposite))
            moved[0] = (piece, beside, opposite)
        moved.append(send_features(payload))
    total = None
    for (first, last), sends in zip(groups, moved):
        count = last - first
        slots_here = 2 * count * capacity
        portion = gather_features([sends])
        if first == 0:
            packed = portion[slots_here:]
            pieces = packed.shape[1] // units_here
            shared_piece = jnp.concatenate(
                [
                    jnp.concatenate(
                        [
                            lax.slice_in_dim(
                                packed,
                                (p * packing + i) * shared_units,
                                (p * packing + i + 1) * shared_units,
                                axis=1,
                            )
                            for p in range(pieces)
                        ],
                        axis=1,
                    )
                    for i in range(packing)
                ],
                axis=0,
            )
            shared = jnp.dot(shared_piece, shared_down, preferred_element_type=jnp.float32)
        result = jnp.dot(portion[:slots_here], local_down, preferred_element_type=jnp.float32)
        result = result * slot_factor[:, first:last].reshape(slots_here, 1)
        result = result.astype(jnp.bfloat16).reshape(2, count, capacity, columns)
        crossed = lax.ppermute(result[1], "ep", sibling)
        summed = jnp.einsum(
            "scr,scd->srd",
            spread[first:last],
            jnp.concatenate([result[0], crossed], axis=1),
            preferred_element_type=jnp.float32,
        )
        for place in range(first, last):
            term = summed[place - first]
            if place > 0:
                term = shifted(term.astype(jnp.bfloat16), -order[place]).astype(jnp.float32)
            total = term if total is None else total + term
    return (attended, (total + shared).astype(jnp.bfloat16))


def shards(
    query_vectors,
    key_vectors,
    value_vectors,
    query_gain,
    key_gain,
    sink_logits,
    moe_rows,
    norm_gain,
    expert_ids,
    route_weights,
    expert_gate,
    expert_up,
    expert_down,
    shared_gate,
    shared_up,
    shared_down,
):
    low, high = borders(key_vectors, value_vectors)

    def attend(after):
        queries, _ = lax.optimization_barrier((query_vectors, after))
        return attend_window(
            queries, key_vectors, value_vectors, low, high, query_gain, key_gain, sink_logits
        )

    moe_args = (
        moe_rows,
        norm_gain,
        expert_ids,
        route_weights,
        expert_gate,
        expert_up,
        expert_down,
        shared_gate,
        shared_up,
        shared_down,
    )
    ep_size = lax.axis_size("ep")
    tokens_here = moe_rows.shape[0]
    few = ep_size * tokens_here <= 3 * tokens_here * TOP_K
    if few and ep_size % 2 == 0 and lax.axis_size("tp") == 4:
        return dense_layer(*moe_args, attend)
    return (attend(moe_rows), routed_layer(*moe_args))


def solution(mesh):
    placed = (
        P("ep", "tp"),
        P("ep", "tp"),
        P("ep", "tp"),
        P(),
        P(),
        P("tp"),
        P("ep", "tp"),
        P(),
        P("ep", None),
        P("ep", None),
        P("ep", None, "tp"),
        P("ep", None, "tp"),
        P("ep", None, "tp"),
        P(None, "tp"),
        P(None, "tp"),
        P(None, "tp"),
    )
    return jax.shard_map(
        shards,
        mesh=mesh,
        in_specs=placed,
        out_specs=(P("ep", "tp"), P("ep", "tp")),
        check_vma=False,
    )
```
